32 devices in a mesh: ep: 16 (over z, y, x), tp: 2 (over core).
Axes of the slice: x: 2, y: 2, z: 4, core: 2. Of those that a mesh axis runs over, the one named last changes fastest.
Arguments:
- inputs: bfloat16 [1024, 2048], P('ep'), may hold values from -6 to 6
- cache_keys: bfloat16 [1024, 2, 64, 1024], P('ep', 'tp'), may hold values from -6 to 6
- cache_values: bfloat16 [1024, 2, 64, 1024], P('ep', 'tp'), may hold values from -12 to 12
- lengths: int32 [1024], P('ep'), may hold values from 1 to 1024, as said below
- query_weight: bfloat16 [2048, 1024], P(None, 'tp'), may hold values from -0.125 to 0.125
- key_weight: bfloat16 [2048, 128], P(None, 'tp'), may hold values from -0.125 to 0.125
- value_weight: bfloat16 [2048, 128], P(None, 'tp'), may hold values from -0.125 to 0.125
- head_bias: float32 [16], P('tp'), may hold values from -7 to -3
- out_weight: bfloat16 [1024, 2048], P('tp'), may hold values from -0.75 to 0.75
- attend_gain: float32 [2048], replicated, may hold values from 0.1 to 1.9
- router_weight: bfloat16 [2048, 16], replicated, may hold values from -0.125 to 0.125
- routes: int32 [1024, 4], P('ep'), may hold values from 0 to 15, all different within a row; in each aligned block of 64 rows (0 to 63, 64 to 127, ...) at most 32 rows name the same one
- expert_gate: bfloat16 [16, 2048, 512], P('ep', None, 'tp'), may hold values from -0.125 to 0.125
- expert_up: bfloat16 [16, 2048, 512], P('ep', None, 'tp'), may hold values from -0.125 to 0.125
- expert_down: bfloat16 [16, 512, 2048], P('ep', 'tp'), may hold values from -0.25 to 0.25
- shared_gate: bfloat16 [2048, 512], P(None, 'tp'), may hold values from -0.125 to 0.125
- shared_up: bfloat16 [2048, 512], P(None, 'tp'), may hold values from -0.125 to 0.125
- shared_down: bfloat16 [512, 2048], P('tp'), may hold values from -0.25 to 0.25
- final_gain: float32 [2048], P('tp'), may hold values from 0.1 to 1.9
Outputs:
- output: bfloat16 [1024, 2048], P('ep', 'tp')
- new_keys: bfloat16 [1024, 128], P('ep', 'tp')
- new_values: bfloat16 [1024, 128], P('ep', 'tp')
The draws below stay inside these ranges and needn't reach their ends.
Inputs may be any that keep to these rules, and one draw needn't show every extreme that they name: `lengths`: some sequence has 1024 filled positions and some other has 1. `routes`: each row names 4 different experts. Among the 64 rows of one index of ep no expert is named more than 32 times; some expert is named exactly 32 times by the rows of some index.
All inputs are finite; a program needn't handle non-finite values.
Results may differ from the reference program's by a relative error of at most 0.015.
Values may be sent and summed in bfloat16 or wider, within the bound.
A program may use at most 128 MiB of HBM per device.

```python
import math
import jax
import jax.numpy as jnp
import numpy as np
from jax import lax

D = 2048
HEAD = 64
Q_HEADS = 16
KV_HEADS = 2
FF_EXP = 512
FF_SH = 512
TOPK = 4
SEQ_DEV = 64
CACHE = 1024
SEQS = 1024
EXPERTS = 16
CAP = 32
N_EP = 16
N_TP = 2


def draw_lengths(key, part):
    first_key = jax.random.fold_in(key, 11)
    second_key = jax.random.fold_in(key, 12)
    third_key = jax.random.fold_in(key, 13)
    blocks = SEQS // SEQ_DEV
    limits = jax.random.randint(first_key, (blocks, 1), CACHE // 8, CACHE + 1)
    spread = jax.random.randint(second_key, (blocks, SEQ_DEV), 0, CACHE)
    filled = (1 + spread % limits).reshape(SEQS)
    order = jax.random.permutation(third_key, SEQS)
    filled = filled.at[order[0]].set(CACHE).at[order[1]].set(1)
    return filled.astype(jnp.int32)


def shard_levels(own_key, shape, cuts, least, top_value):
    loudness = 1.0
    for dim, parts in cuts:
        heights = jax.random.uniform(jax.random.fold_in(jax.random.fold_in(own_key, 6), dim), (parts,), jnp.float32, least / len(cuts), top_value / len(cuts))
        loudness = loudness * jnp.repeat(jnp.exp(heights), shape[dim] // parts).reshape((-1,) + (1,) * (len(shape) - 1 - dim))
    return loudness


def routed_block(stream_key, own, number, rows, amount, top, bound, lean):
    sequence = jax.random.permutation(stream_key, amount)
    heavy_load, common = shares(amount, rows * top, bound, lean, True), shares(amount, rows * top, bound, lean, False)
    places = jnp.arange(amount)

    def named(sizes, offset_by):
        used = int((sizes > 0).sum())
        fixed = max(1, used // 4)
        shifted = fixed + (places - fixed + offset_by * (used - fixed)) % max(1, amount - fixed)
        return jnp.zeros((amount,), jnp.int32).at[sequence[jnp.where(places < fixed, places, shifted)]].set(jnp.asarray(sizes, jnp.int32))

    sizes = jnp.where(number % 4 == 0, named(heavy_load, number // 4), named(common, number - number // 4 - 1))
    mixed = jax.random.permutation(jax.random.fold_in(own, 3), amount)
    giver, taker = mixed[0:amount // 2 * 2:2], mixed[1:amount // 2 * 2:2]
    slack = jnp.minimum(sizes[giver] - 1, bound - sizes[taker]) // 2
    slack = jnp.where((giver == sequence[0]) | (taker == sequence[0]) | (sizes[taker] == 0), 0, jnp.maximum(slack, 0))
    shifted = jax.random.randint(jax.random.fold_in(own, 4), (amount // 2,), 0, 1 << 20) % (slack + 1)
    sizes = sizes.at[giver].add(-shifted).at[taker].add(shifted)
    items = jnp.searchsorted(jnp.cumsum(sizes), jnp.arange(rows * top), side="right").astype(jnp.int32)
    table = items.reshape(top, rows).T
    table = table[jax.random.permutation(jax.random.fold_in(own, 1), rows)]
    offset_by = jax.random.randint(jax.random.fold_in(own, 2), (rows, 1), 0, top)
    return jnp.take_along_axis(table, (jnp.arange(top)[None, :] + offset_by) % top, axis=1)


def shares(amount, total, most, lean, full):
    weights = [(1 << 20) // math.isqrt(rank ** lean) + 1 for rank in range(1, amount + 1)]
    largest = most if full else min(most, max(-(-total // amount), total * weights[0] // sum(weights)))
    least = 1 if total - largest >= amount - 1 else 0
    counts, spare = [largest] + [least] * (amount - 1), total - largest - least * (amount - 1)
    while spare > 0:
        movable = [i for i in range(1, amount) if counts[i] < largest] or [i for i in range(1, amount) if counts[i] < most]
        mass, budget = sum([weights[i] for i in movable]), spare
        for i in movable:
            more = min(most - counts[i], max(1, budget * weights[i] // mass), spare)
            counts[i] = counts[i] + more
            spare = spare - more
    return np.array(counts)


def bell_draw(own_key, shape, scale, limit, split=(), kind=jnp.bfloat16):
    result = jax.random.normal(own_key, shape, jnp.float32) * scale
    if len(split) > 0:
        result = shard_levels(own_key, shape, split, -0.22, 0.18) * result
    return jnp.clip(result, min=-limit, max=limit).astype(kind)


def setup_inputs(seed: int = 0) -> dict:
    seeds = jax.random.split(jax.random.key(seed), 20)
    inputs = bell_draw(seeds[0], (SEQS, D), 1.0, 6.0, ((0, 16),))
    cache_keys = bell_draw(seeds[1], (SEQS, KV_HEADS, HEAD, CACHE), 1.0, 6.0, ((0, 16), (1, 2)))
    cache_values = bell_draw(seeds[2], (SEQS, KV_HEADS, HEAD, CACHE), 2.0, 12.0, ((0, 16), (1, 2)))
    lengths = draw_lengths(jax.random.fold_in(seeds[19], 71), 0)
    query_weight = bell_draw(seeds[4], (D, Q_HEADS * HEAD), D ** -0.5, 0.125, ((1, 2),))
    key_weight = bell_draw(seeds[5], (D, KV_HEADS * HEAD), D ** -0.5, 0.125, ((1, 2),))
    value_weight = bell_draw(seeds[6], (D, KV_HEADS * HEAD), D ** -0.5, 0.125, ((1, 2),))
    head_bias = jnp.clip(-7.0 + 4.0 * jax.random.uniform(seeds[7], (Q_HEADS,), jnp.float32) ** shard_levels(seeds[7], (Q_HEADS,), ((0, 2),), -0.2, 0.2), -7.0, -3.0)
    out_weight = bell_draw(seeds[8], (Q_HEADS * HEAD, D), HEAD ** -0.5, 0.75, ((0, 2),))
    attend_gain = jnp.clip(1.0 + 0.18 * jax.random.normal(seeds[9], (D,), jnp.float32), 0.1, 1.9)
    router_weight = bell_draw(seeds[10], (D, EXPERTS), D ** -0.5, 0.125)
    routes_keys = jax.random.split(jax.random.fold_in(seeds[11], 1), SEQS // SEQ_DEV)
    routes_turns = jax.random.permutation(jax.random.fold_in(seeds[11], 3), SEQS // SEQ_DEV)
    routes = jax.vmap(lambda own, number: routed_block(jax.random.fold_in(seeds[11], 2), own, number, SEQ_DEV, EXPERTS, TOPK, CAP, 2))(routes_keys, routes_turns).reshape((SEQS, TOPK))
    expert_gate = bell_draw(seeds[12], (EXPERTS, D, FF_EXP), D ** -0.5, 0.125, ((0, 16), (2, 2)))
    expert_up = bell_draw(seeds[13], (EXPERTS, D, FF_EXP), D ** -0.5, 0.125, ((0, 16), (2, 2)))
    expert_down = bell_draw(seeds[14], (EXPERTS, FF_EXP, D), FF_EXP ** -0.5, 0.25, ((0, 16), (1, 2)))
    shared_gate = bell_draw(seeds[15], (D, FF_SH), D ** -0.5, 0.125, ((1, 2),))
    shared_up = bell_draw(seeds[16], (D, FF_SH), D ** -0.5, 0.125, ((1, 2),))
    shared_down = bell_draw(seeds[17], (FF_SH, D), FF_SH ** -0.5, 0.25, ((0, 2),))
    final_gain = jnp.clip(1.0 + 0.18 * jax.random.normal(seeds[18], (D,), jnp.float32), 0.1, 1.9)
    return {"inputs": inputs, "cache_keys": cache_keys, "cache_values": cache_values, "lengths": lengths, "query_weight": query_weight, "key_weight": key_weight, "value_weight": value_weight, "head_bias": head_bias, "out_weight": out_weight, "attend_gain": attend_gain, "router_weight": router_weight, "routes": routes, "expert_gate": expert_gate, "expert_up": expert_up, "expert_down": expert_down, "shared_gate": shared_gate, "shared_up": shared_up, "shared_down": shared_down, "final_gain": final_gain}


RESIDUAL_SCALE = 2.0 ** 0.25
ROUTE_SCALE = 2.5
NORM_EPS = 1e-05

def layer_norm(values, gain_vec):
    row_mean = lax.optimization_barrier(jnp.mean(values, axis=-1, keepdims=True))
    centered = values - row_mean
    row_var = lax.optimization_barrier(jnp.mean(centered * centered, axis=-1, keepdims=True))
    return centered * lax.rsqrt(row_var + NORM_EPS) * gain_vec

def split_sum(inner_rows, weight_rows, pieces):
    total_rows, inner_width = inner_rows.shape
    left_parts = inner_rows.reshape(total_rows, pieces, inner_width // pieces).astype(jnp.float32)
    right_parts = weight_rows.reshape(pieces, inner_width // pieces, -1).astype(jnp.float32)
    partial_value = jnp.einsum('rpf,pfd->prd', left_parts, right_parts)
    rounded = lax.optimization_barrier(partial_value.astype(jnp.bfloat16))
    return lax.optimization_barrier(jnp.sum(rounded.astype(jnp.float32), axis=0))

def reference(inputs, cache_keys, cache_values, lengths, query_weight, key_weight, value_weight, head_bias, out_weight, attend_gain, router_weight, routes, expert_gate, expert_up, expert_down, shared_gate, shared_up, shared_down, final_gain):
    groups = Q_HEADS // KV_HEADS
    query = jnp.dot(inputs, query_weight, preferred_element_type=jnp.float32).astype(jnp.bfloat16)
    new_keys = jnp.dot(inputs, key_weight, preferred_element_type=jnp.float32).astype(jnp.bfloat16)
    new_values = jnp.dot(inputs, value_weight, preferred_element_type=jnp.float32).astype(jnp.bfloat16)
    query_heads = query.reshape(SEQS, KV_HEADS, groups, HEAD).astype(jnp.float32)
    scores = jnp.einsum('skgd,skdc->skgc', query_heads, cache_keys.astype(jnp.float32)) * HEAD ** (-0.5)
    scores = scores + head_bias.reshape(KV_HEADS, groups)[None, :, :, None]
    positions = jnp.arange(CACHE, dtype=jnp.int32)
    usable = positions[None, None, None, :] < lengths[:, None, None, None]
    log_keep = jnp.where(usable, jax.nn.log_sigmoid(-scores), 0.0)
    later_sum = lax.cumsum(log_keep, axis=3, reverse=True) - log_keep
    stick_weight = jnp.where(usable, jnp.exp(jax.nn.log_sigmoid(scores) + later_sum), 0.0).astype(jnp.bfloat16)
    attended = jnp.einsum('skgc,skdc->skgd', stick_weight.astype(jnp.float32), cache_values.astype(jnp.float32))
    attended = attended.astype(jnp.bfloat16).reshape(SEQS, Q_HEADS * HEAD)
    attention = split_sum(attended, out_weight, N_TP)
    hidden = layer_norm(RESIDUAL_SCALE * inputs.astype(jnp.float32) + attention, attend_gain).astype(jnp.bfloat16)
    router_probs = jax.nn.sigmoid(jnp.dot(hidden, router_weight, preferred_element_type=jnp.float32))
    chosen = jnp.take_along_axis(router_probs, routes, axis=1)
    route_weights = ROUTE_SCALE * chosen / lax.optimization_barrier(jnp.sum(chosen, axis=1, keepdims=True))
    block_routes = routes.reshape(N_EP, SEQ_DEV * TOPK)
    onehot_rows = (block_routes[:, :, None] == jnp.arange(EXPERTS, dtype=jnp.int32)[None, None, :]).astype(jnp.int32)
    earlier_count = jnp.cumsum(onehot_rows, axis=1) - onehot_rows
    slot_index = lax.optimization_barrier(jnp.sum(earlier_count * onehot_rows, axis=2))
    column = (jnp.arange(N_EP, dtype=jnp.int32)[:, None] * CAP + slot_index).reshape(-1).astype(jnp.int32)
    flat_routes = routes.reshape(-1)
    token_index = jnp.repeat(jnp.arange(SEQS, dtype=jnp.int32), TOPK)
    slot_table = jnp.full((EXPERTS, N_EP * CAP), SEQS, jnp.int32).at[flat_routes, column].set(token_index)
    padded_rows = jnp.concatenate([hidden, jnp.zeros((1, D), jnp.bfloat16)], axis=0)

    def one_expert(packed):
        row_index, gate_mat, up_mat, down_mat = packed
        rows = padded_rows[row_index]
        gate_act = jnp.dot(rows, gate_mat, preferred_element_type=jnp.float32)
        up_act = jnp.dot(rows, up_mat, preferred_element_type=jnp.float32)
        inner = (jax.nn.silu(gate_act) * up_act).astype(jnp.bfloat16)
        return split_sum(inner, down_mat, N_TP).astype(jnp.bfloat16)
    results = lax.map(one_expert, (slot_table, expert_gate, expert_up, expert_down))
    picked = results[flat_routes, column].astype(jnp.float32).reshape(SEQS, TOPK, D)
    routed = lax.optimization_barrier(jnp.sum(route_weights[:, :, None] * picked, axis=1))
    shared_g = jnp.dot(hidden, shared_gate, preferred_element_type=jnp.float32)
    shared_u = jnp.dot(hidden, shared_up, preferred_element_type=jnp.float32)
    shared_inner = (jax.nn.silu(shared_g) * shared_u).astype(jnp.bfloat16)
    shared_result = split_sum(shared_inner, shared_down, N_TP)
    mixed_rows = RESIDUAL_SCALE * hidden.astype(jnp.float32) + routed + shared_result
    output = layer_norm(mixed_rows, final_gain).astype(jnp.bfloat16)
    return (output, new_keys, new_values)
```

```python
import functools
import math

import jax
import jax.numpy as jnp
from jax import lax
from jax.experimental import pallas as pl
from jax.experimental.pallas import tpu as pltpu
from jax.sharding import PartitionSpec as P

RESIDUAL_SCALE = 2.0**0.25
ROUTE_SCALE = 2.5
NORM_EPS = 1e-05


def layer_norm(values, gain_vec):
    row_mean = jnp.mean(values, axis=-1, keepdims=True)
    centered = values - row_mean
    row_var = jnp.mean(centered * centered, axis=-1, keepdims=True)
    return centered * lax.rsqrt(row_var + NORM_EPS) * gain_vec


def strictly_later(size):
    row_pos = lax.broadcasted_iota(jnp.int32, (size, size), 0)
    col_pos = lax.broadcasted_iota(jnp.int32, (size, size), 1)
    return (row_pos > col_pos).astype(jnp.float32)


def later_totals(log_keep):
    lead = log_keep.shape[:-1]
    length = log_keep.shape[-1]
    block_size = math.gcd(length, 128)
    block_count = length // block_size
    blocked = log_keep.reshape(lead + (block_count, block_size))
    inside = jnp.einsum(
        "...bi,ic->...bc", blocked, strictly_later(block_size), precision=lax.Precision.HIGHEST
    )
    block_total = jnp.sum(blocked, axis=-1)
    after = jnp.einsum(
        "...i,ic->...c", block_total, strictly_later(block_count), precision=lax.Precision.HIGHEST
    )
    return (inside + after[..., None]).reshape(lead + (length,))


LANES = 128
VMEM_BYTES = 67043328
BF16 = jnp.bfloat16
F32 = jnp.float32


def grid_of(count):
    side = round(count ** (1.0 / 3.0))
    if side**3 == count:
        return side, side, side
    if count % 4 == 0:
        return count // 4, 2, 2
    return count, 1, 1


def moe_kernel(
    dims,
    part_ref,
    inputs_ref,
    mask_ref,
    attend_gain_ref,
    final_gain_ref,
    router_hbm,
    gate_hbm,
    up_hbm,
    down_hbm,
    sgate_hbm,
    sup_hbm,
    sdown_hbm,
    out_ref,
    part_in,
    rows_all,
    router_w,
    gate_w,
    up_w,
    down_w,
    sgate_w,
    sup_w,
    sdown_w,
    own_sum,
    pair_out,
    pair_in,
    shared_mine,
    first_a,
    first_b,
    second_a,
    second_b,
    third,
    stats_out,
    stats_in,
    load_sem,
    send_sem,
    part_sem,
    full_sem,
    a_sem,
    b_sem,
    pf_sem,
    pa_sem,
    pb_sem,
    pair_sem,
    fa_sem,
    fb_sem,
    sa_sem,
    sb_sem,
    third_sem,
    stats_sem,
):
    nz, ny, nx = dims
    rows, width = inputs_ref.shape
    half = rows // 2
    dh = width // 2
    dq = dh // 2
    plane = ny * nx * rows
    core = lax.axis_index("tp")
    other = 1 - core
    me = lax.axis_index("ep")
    x = me % nx
    y = (me // nx) % ny
    z = me // (nx * ny)

    def index(dz, dy, dx):
        return (((z + nz - dz) % nz) * ny + (y + ny - dy) % ny) * nx + (x + nx - dx) % nx

    def rel(dz, dy, dx):
        return (dz * ny + dy) * nx + dx

    def to_z(step):
        return {"ep": (((z + step) % nz) * ny + y) * nx + x}

    def to_y(step):
        return {"ep": (z * ny + (y + step) % ny) * nx + x}

    def to_x(step):
        return {"ep": (z * ny + y) * nx + (x + step) % nx}

    partner = {"tp": other}
    loads = []
    for i, (src, dst) in enumerate(
        (
            (router_hbm, router_w),
            (sgate_hbm, sgate_w),
            (sup_hbm, sup_w),
            (sdown_hbm, sdown_w),
            (gate_hbm, gate_w),
            (up_hbm, up_w),
            (down_hbm, down_w),
        )
    ):
        copy = pltpu.make_async_copy(src, dst, load_sem.at[i])
        copy.start()
        loads.append(copy)

    barrier = pltpu.get_barrier_semaphore()
    greeted = [partner]
    greeted += [to_z(i) for i in range(1, nz)]
    greeted += [to_y(i) for i in range(1, ny)]
    greeted += [to_x(i) for i in range(1, nx)]
    for device in greeted:
        pl.semaphore_signal(barrier, inc=1, device_id=device, device_id_type=pl.DeviceIdType.MESH)
    pl.semaphore_wait(barrier, len(greeted))

    sent = []

    def remote(src, dst, recv, device):
        copy = pltpu.make_async_remote_copy(
            src_ref=src,
            dst_ref=dst,
            send_sem=send_sem.at[len(sent)],
            recv_sem=recv,
            device_id=device,
            device_id_type=pl.DeviceIdType.MESH,
        )
        copy.start()
        sent.append(copy)

    def arrived(dst, recv):
        pltpu.make_async_remote_copy(
            src_ref=dst,
            dst_ref=dst,
            send_sem=send_sem.at[0],
            recv_sem=recv,
            device_id=partner,
            device_id_type=pl.DeviceIdType.MESH,
        ).wait_recv()

    def mult(value, by):
        return pl.multiple_of(value, by)

    remote(part_ref.at[pl.ds(mult(other * half, half), half)], part_in, part_sem.at[0], partner)
    arrived(part_in, part_sem.at[0])
    own_half = pl.ds(mult(core * half, half), half)
    attention = part_ref[own_half, :].astype(F32) + part_in[...].astype(F32)
    hidden = layer_norm(
        RESIDUAL_SCALE * inputs_ref[own_half, :].astype(F32) + attention, attend_gain_ref[...]
    ).astype(BF16)
    loads[0].wait()
    probs = jax.nn.sigmoid(jnp.dot(hidden, router_w[...], preferred_element_type=F32))
    chosen = probs * mask_ref[own_half, :]
    weights = ROUTE_SCALE * chosen / jnp.sum(chosen, axis=1, keepdims=True)
    mine = pl.ds(mult(me * rows + core * half, half), half)
    rows_all[mine, pl.ds(0, width)] = hidden
    rows_all[mine, pl.ds(width, LANES)] = weights.astype(BF16)

    full_cols = pl.ds(0, width + LANES)
    a_cols = pl.ds(0, dh)
    b_cols = pl.ds(dh, dh + LANES)

    def slot(dz, dy, dx, cols, who=core):
        return rows_all.at[pl.ds(mult(index(dz, dy, dx) * rows + who * half, half), half), cols]

    def spread(dz, dy, dx, cols, targets, sems):
        block = slot(dz, dy, dx, cols)
        for device, sem_index in targets:
            remote(block, block, sems.at[sem_index], device)

    def have_full(dz):
        spread(dz, 0, 0, a_cols, [(to_y(i), rel(dz, i, 0)) for i in range(1, ny)], a_sem)
        spread(dz, 0, 0, b_cols, [(to_x(i), rel(dz, 0, i)) for i in range(1, nx)], b_sem)
        spread(dz, 0, 0, a_cols, [(to_x(i), rel(dz, 0, i)) for i in range(1, nx)], a_sem)
        spread(dz, 0, 0, b_cols, [(to_y(i), rel(dz, i, 0)) for i in range(1, ny)], b_sem)
        spread(dz, 0, 0, full_cols, [(partner, rel(dz, 0, 0))], pf_sem)

    def have_middle(dz):
        for dy in range(1, ny):
            arrived(slot(dz, dy, 0, a_cols), a_sem.at[rel(dz, dy, 0)])
            spread(dz, dy, 0, a_cols, [(to_x(i), rel(dz, dy, i)) for i in range(1, nx)], a_sem)
            spread(dz, dy, 0, a_cols, [(partner, rel(dz, dy, 0))], pa_sem)
        for dx in range(1, nx):
            arrived(slot(dz, 0, dx, b_cols), b_sem.at[rel(dz, 0, dx)])
            spread(dz, 0, dx, b_cols, [(to_y(i), rel(dz, i, dx)) for i in range(1, ny)], b_sem)
            spread(dz, 0, dx, b_cols, [(partner, rel(dz, 0, dx))], pb_sem)

    def have_last(dz):
        for dy in range(ny):
            for dx in range(nx):
                if dx > 0:
                    arrived(slot(dz, dy, dx, a_cols), a_sem.at[rel(dz, dy, dx)])
                    spread(dz, dy, dx, a_cols, [(partner, rel(dz, dy, dx))], pa_sem)
                if dy > 0:
                    arrived(slot(dz, dy, dx, b_cols), b_sem.at[rel(dz, dy, dx)])
                    spread(dz, dy, dx, b_cols, [(partner, rel(dz, dy, dx))], pb_sem)
        for dy in range(ny):
            for dx in range(nx):
                if dy + dx == 0:
                    if dz > 0:
                        arrived(slot(dz, 0, 0, full_cols, other), pf_sem.at[rel(dz, 0, 0)])
                    continue
                arrived(slot(dz, dy, dx, a_cols, other), pa_sem.at[rel(dz, dy, dx)])
                arrived(slot(dz, dy, dx, b_cols, other), pb_sem.at[rel(dz, dy, dx)])

    spread(0, 0, 0, full_cols, [(to_z(i), rel(i, 0, 0)) for i in range(1, nz)], full_sem)
    have_full(0)
    for dz in range(1, nz):
        arrived(slot(dz, 0, 0, full_cols), full_sem.at[rel(dz, 0, 0)])
        have_full(dz)
        have_middle(dz - 1)
    arrived(slot(0, 0, 0, full_cols, other), pf_sem.at[rel(0, 0, 0)])

    keep_cols = pl.ds(mult(core * dh, dh), dh)
    give_cols = pl.ds(mult(other * dh, dh), dh)
    own_rows = pl.ds(mult(me * rows, rows), rows)
    for copy in loads[1:]:
        copy.wait()
    own_hidden = rows_all[own_rows, pl.ds(0, width)]
    shared_g = jnp.dot(own_hidden, sgate_w[...], preferred_element_type=F32)
    shared_u = jnp.dot(own_hidden, sup_w[...], preferred_element_type=F32)
    shared_inner = (jax.nn.silu(shared_g) * shared_u).astype(BF16)
    shared_mine[...] = jnp.dot(shared_inner, sdown_w[:, keep_cols], preferred_element_type=F32)
    shared_give = jnp.dot(shared_inner, sdown_w[:, give_cols], preferred_element_type=F32)
    have_middle(nz - 1)

    chunk = math.gcd(plane, 256)

    def plane_start(dz):
        return ((z + nz - dz) % nz) * plane

    def compute(dz):
        start = plane_start(dz)

        def one(i, carry):
            part = pl.ds(mult(start + i * chunk, chunk), chunk)
            tokens = rows_all[part, pl.ds(0, width)]
            gate_act = jnp.dot(tokens, gate_w[...], preferred_element_type=F32)
            up_act = jnp.dot(tokens, up_w[...], preferred_element_type=F32)
            inner = (jax.nn.silu(gate_act) * up_act).astype(BF16)
            table = rows_all[part, pl.ds(width, LANES)].astype(F32)
            lane = lax.broadcasted_iota(jnp.int32, (chunk, LANES), 1)
            scale = jnp.sum(jnp.where(lane == me, table, 0.0), axis=1, keepdims=True)
            pair_out[part, :] = (
                scale * jnp.dot(inner, down_w[:, give_cols], preferred_element_type=F32)
            ).astype(BF16)
            own_sum[part, :] = (
                scale * jnp.dot(inner, down_w[:, keep_cols], preferred_element_type=F32)
            ).astype(BF16)
            return carry

        lax.fori_loop(0, plane // chunk, one, 0)
        if dz == 0:
            pair_out[own_rows, :] = (pair_out[own_rows, :].astype(F32) + shared_give).astype(BF16)
        whole = pl.ds(mult(start, plane), plane)
        remote(pair_out.at[whole], pair_in.at[whole], pair_sem.at[dz], partner)

    a_part = pl.ds(0, dq)
    b_part = pl.ds(dq, dq)

    def block(dz, dy, dx):
        return pl.ds(mult(index(dz, dy, dx) * rows, rows), rows)

    def first(dz):
        whole = pl.ds(mult(plane_start(dz), plane), plane)
        arrived(pair_in.at[whole], pair_sem.at[dz])

        def one(i, carry):
            part = pl.ds(mult(plane_start(dz) + i * rows, rows), rows)
            own_sum[part, :] = (
                own_sum[part, :].astype(F32) + pair_in[part, :].astype(F32)
            ).astype(BF16)
            return carry

        lax.fori_loop(0, plane // rows, one, 0)
        for step in range(1, nx):
            for dy in range(ny - 1, -1, -1):
                at = (dz * (nx - 1) + step - 1) * ny + dy
                remote(
                    own_sum.at[block(dz, dy, nx - step), a_part],
                    first_a.at[at],
                    fa_sem.at[at],
                    to_x(step),
                )
        for step in range(1, ny):
            for dx in range(nx - 1, -1, -1):
                at = (dz * (ny - 1) + step - 1) * nx + dx
                remote(
                    own_sum.at[block(dz, ny - step, dx), b_part],
                    first_b.at[at],
                    fb_sem.at[at],
                    to_y(step),
                )

    def add_in(where, cols, buffer, sems, places):
        total = own_sum[where, cols].astype(F32)
        for at in places:
            arrived(buffer.at[at], sems.at[at])
            total = total + buffer[at].astype(F32)
        own_sum[where, cols] = total.astype(BF16)

    def second(dz):
        for dy in range(ny - 1, -1, -1):
            places = [(dz * (nx - 1) + step - 1) * ny + dy for step in range(1, nx)]
            add_in(block(dz, dy, 0), a_part, first_a, fa_sem, places)
            if dy > 0:
                at = dz * (ny - 1) + ny - dy - 1
                remote(
                    own_sum.at[block(dz, dy, 0), a_part],
                    second_a.at[at],
                    sa_sem.at[at],
                    to_y(ny - dy),
                )
        for dx in range(nx - 1, -1, -1):
            places = [(dz * (ny - 1) + step - 1) * nx + dx for step in range(1, ny)]
            add_in(block(dz, 0, dx), b_part, first_b, fb_sem, places)
            if dx > 0:
                at = dz * (nx - 1) + nx - dx - 1
                remote(
                    own_sum.at[block(dz, 0, dx), b_part],
                    second_b.at[at],
                    sb_sem.at[at],
                    to_x(nx - dx),
                )

    def last(dz):
        places = [dz * (ny - 1) + step - 1 for step in range(1, ny)]
        add_in(block(dz, 0, 0), a_part, second_a, sa_sem, places)
        places = [dz * (nx - 1) + step - 1 for step in range(1, nx)]
        add_in(block(dz, 0, 0), b_part, second_b, sb_sem, places)
        if dz > 0:
            remote(
                own_sum.at[block(dz, 0, 0)], third.at[dz - 1], third_sem.at[dz - 1], to_z(nz - dz)
            )

    order = list(range(nz))
    for k in range(nz + 3):
        if k < nz:
            have_last(order[k])
            compute(order[k])
        if 1 <= k < nz + 1:
            first(order[k - 1])
        if 2 <= k < nz + 2:
            second(order[k - 2])
        if 3 <= k:
            last(order[k - 3])

    total = own_sum[own_rows, :].astype(F32) + shared_mine[...]
    total = total + RESIDUAL_SCALE * rows_all[own_rows, keep_cols].astype(F32)
    for i in range(nz - 1):
        arrived(third.at[i], third_sem.at[i])
        total = total + third[i].astype(F32)
    lane = lax.broadcasted_iota(jnp.int32, (rows, LANES), 1)
    sum_one = jnp.sum(total, axis=1, keepdims=True)
    sum_two = jnp.sum(total * total, axis=1, keepdims=True)
    stats_out[...] = jnp.where(lane == 0, sum_one, sum_two)
    remote(stats_out, stats_in, stats_sem.at[0], partner)
    arrived(stats_in, stats_sem.at[0])
    row_mean = (sum_one + stats_in[:, 0:1]) / width
    row_var = (sum_two + stats_in[:, 1:2]) / width - row_mean * row_mean
    normed = (total - row_mean) * lax.rsqrt(row_var + NORM_EPS)
    out_ref[...] = (normed * final_gain_ref[...]).astype(BF16)
    for copy in sent:
        copy.wait_send()


def moe_layer(
    count, part, inputs, mask, attend_gain, final_gain, router, gate, up, down, sgate, sup, sdown
):
    dims = grid_of(count)
    nz, ny, nx = dims
    rows, width = inputs.shape
    half = rows // 2
    dh = width // 2
    dq = dh // 2
    everyone = count * rows
    sends = 3 + (nz - 1) + 2 * (count + nz) + nz * (nx - 1 + ny - 1) * 2 + 2 * count
    sends += 2 * nz * ny * nx + nz + 2 * nz * (ny + nx + ny * nx) + nz
    vmem = pl.BlockSpec(memory_space=pltpu.VMEM)
    anywhere = pl.BlockSpec(memory_space=pl.ANY)
    n1a, n1b = max(1, nz * (nx - 1) * ny), max(1, nz * (ny - 1) * nx)
    n2a, n2b = max(1, nz * (ny - 1)), max(1, nz * (nx - 1))
    n3 = max(1, nz - 1)
    dma = pltpu.SemaphoreType.DMA
    return pl.pallas_call(
        functools.partial(moe_kernel, dims),
        out_shape=jax.ShapeDtypeStruct((rows, dh), BF16),
        in_specs=[vmem] * 5 + [anywhere] * 7,
        out_specs=vmem,
        scratch_shapes=[
            pltpu.VMEM((half, width), BF16),
            pltpu.VMEM((everyone, width + LANES), BF16),
            pltpu.VMEM(router.shape, BF16),
            pltpu.VMEM(gate.shape, BF16),
            pltpu.VMEM(up.shape, BF16),
            pltpu.VMEM(down.shape, BF16),
            pltpu.VMEM(sgate.shape, BF16),
            pltpu.VMEM(sup.shape, BF16),
            pltpu.VMEM(sdown.shape, BF16),
            pltpu.VMEM((everyone, dh), BF16),
            pltpu.VMEM((everyone, dh), BF16),
            pltpu.VMEM((everyone, dh), BF16),
            pltpu.VMEM((rows, dh), F32),
            pltpu.VMEM((n1a, rows, dq), BF16),
            pltpu.VMEM((n1b, rows, dq), BF16),
            pltpu.VMEM((n2a, rows, dq), BF16),
            pltpu.VMEM((n2b, rows, dq), BF16),
            pltpu.VMEM((n3, rows, dh), BF16),
            pltpu.VMEM((rows, LANES), F32),
            pltpu.VMEM((rows, LANES), F32),
            dma((7,)),
            dma((sends,)),
            dma((1,)),
            dma((count,)),
            dma((count,)),
            dma((count,)),
            dma((count,)),
            dma((count,)),
            dma((count,)),
            dma((nz,)),
            dma((n1a,)),
            dma((n1b,)),
            dma((n2a,)),
            dma((n2b,)),
            dma((n3,)),
            dma((1,)),
        ],
        compiler_params=pltpu.CompilerParams(
            collective_id=0, has_side_effects=True, vmem_limit_bytes=VMEM_BYTES
        ),
    )(part, inputs, mask, attend_gain, final_gain, router, gate, up, down, sgate, sup, sdown)


def on_device(
    inputs,
    cache_keys,
    cache_values,
    lengths,
    query_weight,
    key_weight,
    value_weight,
    head_bias,
    out_weight,
    attend_gain,
    router_weight,
    routes,
    expert_gate,
    expert_up,
    expert_down,
    shared_gate,
    shared_up,
    shared_down,
    final_gain,
):
    seq_count, model_width = inputs.shape
    key_heads, head_size, cache_length = cache_keys.shape[1:]
    query_heads = head_bias.shape[0]
    groups = query_heads // key_heads
    experts = router_weight.shape[1]
    query = jnp.dot(inputs, query_weight, preferred_element_type=jnp.float32).astype(jnp.bfloat16)
    query = query.reshape(seq_count, key_heads, groups, head_size)
    new_keys = jnp.dot(inputs, key_weight, preferred_element_type=jnp.float32).astype(jnp.bfloat16)
    new_values = jnp.dot(inputs, value_weight, preferred_element_type=jnp.float32).astype(
        jnp.bfloat16
    )
    scores = jnp.einsum("skgd,skdc->skgc", query, cache_keys, preferred_element_type=jnp.float32)
    scores = scores * head_size ** (-0.5) + head_bias.reshape(key_heads, groups)[None, :, :, None]
    usable = (
        lax.broadcasted_iota(jnp.int32, (1, 1, 1, cache_length), 3) < lengths[:, None, None, None]
    )
    log_keep = jnp.where(usable, jax.nn.log_sigmoid(-scores), 0.0)
    later_sum = later_totals(log_keep)
    stick_weight = jnp.where(usable, jnp.exp(jax.nn.log_sigmoid(scores) + later_sum), 0.0).astype(
        jnp.bfloat16
    )
    attended = jnp.einsum(
        "skgc,skdc->skgd", stick_weight, cache_values, preferred_element_type=jnp.float32
    )
    attended = attended.astype(jnp.bfloat16).reshape(seq_count, query_heads * head_size)
    part = jnp.dot(attended, out_weight, preferred_element_type=jnp.float32).astype(jnp.bfloat16)
    lanes = lax.broadcasted_iota(jnp.int32, (1, 1, LANES), 2)
    mask = jnp.sum((routes[:, :, None] == lanes).astype(jnp.float32), axis=1)
    router = jnp.pad(router_weight, ((0, 0), (0, LANES - experts)))
    output = moe_layer(
        lax.axis_size("ep"),
        part,
        inputs,
        mask,
        attend_gain[None, :],
        final_gain[None, :],
        router,
        expert_gate[0],
        expert_up[0],
        expert_down[0],
        shared_gate,
        shared_up,
        shared_down,
    )
    return (output, new_keys, new_values)


def solution(mesh):
    placed = (
        P("ep", None),
        P("ep", "tp", None, None),
        P("ep", "tp", None, None),
        P("ep"),
        P(None, "tp"),
        P(None, "tp"),
        P(None, "tp"),
        P("tp"),
        P("tp", None),
        P(),
        P(),
        P("ep", None),
        P("ep", None, "tp"),
        P("ep", None, "tp"),
        P("ep", "tp", None),
        P(None, "tp"),
        P(None, "tp"),
        P("tp", None),
        P("tp"),
    )
    return jax.shard_map(
        on_device,
        mesh=mesh,
        in_specs=placed,
        out_specs=(P("ep", "tp"), P("ep", "tp"), P("ep", "tp")),
        check_vma=False,
    )
```
